128 devices in a mesh: ep: 16 (over z, x), tp: 8 (over y, core).
Axes of the slice: x: 4, y: 4, z: 4, core: 2. Of those that a mesh axis runs over, the one named last changes fastest.
Arguments:
- tokens: bfloat16 [512, 2048], P('ep'), may hold values from -6 to 6
- norm_gain: float32 [2048], replicated, may hold values from 0.1 to 1.9
- norm_bias: float32 [2048], replicated, may hold values from -3 to 3
- routes: int32 [512, 4], P('ep'), may hold values from 0 to 15, all different within a row; in each aligned block of 32 rows (0 to 31, 32 to 63, ...) at most 16 rows name the same one
- route_weights: float32 [512, 4], P('ep'), may hold values from 0.2 to 1
- gate_w: bfloat16 [16, 2048, 4096], P('ep', None, 'tp'), may hold values from -0.125 to 0.125
- up_w: bfloat16 [16, 2048, 4096], P('ep', None, 'tp'), may hold values from -0.125 to 0.125
- down_w: bfloat16 [16, 4096, 2048], P('ep', 'tp'), may hold values from -0.09375 to 0.09375
Outputs:
- mixed: bfloat16 [512, 2048], P('ep', 'tp')
The draws below stay inside these ranges and needn't reach their ends.
Inputs may be any that keep to these rules, and one draw needn't show every extreme that they name: `routes`: the 4 experts of a token differ; the rows of one index of ep name no expert more than 16 times, and in every draw some index of ep names some expert exactly 16 times.
All inputs are finite; a program needn't handle non-finite values.
Results may differ from the reference program's by a relative error of at most 0.017.
Values may be sent and summed in bfloat16 or wider, within the bound.
A program may use at most 64 MiB of HBM per device.

```python
import math
import jax
import jax.numpy as jnp
import numpy as np
from jax import lax

D = 2048
FF = 4096
TOPK = 4
TOK_DEV = 32
EXPERTS = 16
CAP = 16
TOKENS = 512
N_TP = 8


def block_scale(rng, dims, shards, smallest, top_value):
    def one(position, parts):
        heights = jax.random.uniform(jax.random.fold_in(jax.random.fold_in(rng, 6), position), (parts,), jnp.float32, smallest / len(shards), top_value / len(shards))
        return jnp.repeat(jnp.exp(heights), dims[position] // parts).reshape((-1,) + (1,) * (len(dims) - position - 1))

    level = one(*shards[0])
    for cut in shards[1:]:
        level = level * one(*cut)
    return level


def deal_out(own_key, own, number, rows, number_of, top, bound, lean):
    sequence = jax.random.permutation(own_key, number_of)
    crowded, common = shares(number_of, rows * top, bound, lean, True), shares(number_of, rows * top, bound, lean, False)
    places = jnp.arange(number_of)

    def named(tallies, turn):
        used = int((tallies > 0).sum())
        fixed = max(1, used // 4)
        moved = fixed + (places - fixed + turn * (used - fixed)) % max(1, number_of - fixed)
        return jnp.zeros((number_of,), jnp.int32).at[sequence[jnp.where(places < fixed, places, moved)]].set(jnp.asarray(tallies, jnp.int32))

    tallies = jnp.where(number % 4 == 0, named(crowded, number // 4), named(common, number - number // 4 - 1))
    mixed = jax.random.permutation(jax.random.fold_in(own, 3), number_of)
    donor, sink = mixed[0:number_of // 2 * 2:2], mixed[1:number_of // 2 * 2:2]
    slack = jnp.minimum(tallies[donor] - 1, bound - tallies[sink]) // 2
    slack = jnp.where((donor == sequence[0]) | (sink == sequence[0]) | (tallies[sink] == 0), 0, jnp.maximum(slack, 0))
    moved = jax.random.randint(jax.random.fold_in(own, 4), (number_of // 2,), 0, 1 << 20) % (slack + 1)
    tallies = tallies.at[donor].add(-moved).at[sink].add(moved)
    labels = jnp.searchsorted(jnp.cumsum(tallies), jnp.arange(rows * top), side="right").astype(jnp.int32)
    listing = labels.reshape(top, rows).T
    listing = listing[jax.random.permutation(jax.random.fold_in(own, 1), rows)]
    turn = jax.random.randint(jax.random.fold_in(own, 2), (rows, 1), 0, top)
    return jnp.take_along_axis(listing, (jnp.arange(top)[None, :] + turn) % top, axis=1)


def shares(count, total, reach, slope, full):
    portions = [(1 << 20) // math.isqrt(rank ** slope) + 1 for rank in range(1, count + 1)]
    largest = reach if full else min(reach, max(-(-total // count), total * portions[0] // sum(portions)))
    least = 1 if total - largest >= count - 1 else 0
    counts, rest = [largest] + [least] * (count - 1), total - largest - least * (count - 1)
    while rest > 0:
        candidates = [i for i in range(1, count) if counts[i] < largest] or [i for i in range(1, count) if counts[i] < reach]
        pool, budget = sum([portions[i] for i in candidates]), rest
        for i in candidates:
            more = min(reach - counts[i], max(1, budget * portions[i] // pool), rest)
            counts[i] = counts[i] + more
            rest = rest - more
    return np.array(counts)


def scatter_about(own_key, shape, spread, most, shards=(), held_as=jnp.bfloat16):
    level = block_scale(own_key, shape, shards, -0.22, 0.18) if shards else 1.0
    drawn = jax.random.normal(own_key, shape, jnp.float32) * spread * level
    return jnp.minimum(jnp.maximum(drawn, -most), most).astype(held_as)


def setup_inputs(seed: int = 0) -> dict:
    splits = jax.random.split(jax.random.key(seed), 9)
    tokens = scatter_about(splits[0], (TOKENS, D), 1.0, 6.0, ((0, 16),))
    norm_gain = jnp.clip(1.0 + 0.18 * jax.random.normal(splits[1], (D,), jnp.float32), 0.1, 1.9)
    norm_bias = scatter_about(splits[2], (D,), 0.5, 3.0, (), jnp.float32)
    routes_keys = jax.random.split(jax.random.fold_in(splits[3], 1), TOKENS // TOK_DEV)
    routes_turns = jax.random.permutation(jax.random.fold_in(splits[3], 3), TOKENS // TOK_DEV)
    routes = jax.vmap(lambda own, number: deal_out(jax.random.fold_in(splits[3], 2), own, number, TOK_DEV, EXPERTS, TOPK, CAP, 2))(routes_keys, routes_turns).reshape((TOKENS, TOPK))
    route_weights = jnp.clip(0.2 + 0.8 * jax.random.uniform(splits[4], (TOKENS, TOPK), jnp.float32) ** block_scale(splits[4], (TOKENS, TOPK), ((0, 16),), -0.2, 0.2), 0.2, 1.0)
    gate_w = scatter_about(splits[5], (EXPERTS, D, FF), D ** -0.5, 0.125, ((0, 16), (2, 8)))
    up_w = scatter_about(splits[6], (EXPERTS, D, FF), D ** -0.5, 0.125, ((0, 16), (2, 8)))
    down_w = scatter_about(splits[7], (EXPERTS, FF, D), FF ** -0.5, 0.09375, ((0, 16), (1, 8)))
    return {"tokens": tokens, "norm_gain": norm_gain, "norm_bias": norm_bias, "routes": routes, "route_weights": route_weights, "gate_w": gate_w, "up_w": up_w, "down_w": down_w}


def layer_norm(tokens, norm_gain, norm_bias):
    values = tokens.astype(jnp.float32)
    centred = values - lax.optimization_barrier(jnp.mean(values, axis=-1, keepdims=True))
    variance = lax.optimization_barrier(jnp.mean(centred * centred, axis=-1, keepdims=True))
    return (centred * lax.rsqrt(variance + 1e-05) * norm_gain + norm_bias).astype(jnp.bfloat16)

def reference(tokens, norm_gain, norm_bias, routes, route_weights, gate_w, up_w, down_w):
    normed = layer_norm(tokens, norm_gain, norm_bias)
    groups = N_TP
    width = down_w.shape[2]
    hidden_units = down_w.shape[1]

    def one_expert(weights):
        gate_one, up_one, down_one = weights
        gate = jnp.dot(normed, gate_one, preferred_element_type=jnp.float32)
        up = jnp.dot(normed, up_one, preferred_element_type=jnp.float32)
        hidden = (jax.nn.silu(gate) * up).astype(jnp.bfloat16)
        hidden_groups = hidden.reshape(hidden.shape[0], groups, hidden_units // groups).astype(jnp.float32)
        down_groups = down_one.reshape(groups, hidden_units // groups, width).astype(jnp.float32)
        partial_sums = jnp.einsum('tgf,gfd->gtd', hidden_groups, down_groups).astype(jnp.bfloat16)
        return lax.optimization_barrier(jnp.sum(partial_sums.astype(jnp.float32), axis=0)).astype(jnp.bfloat16)
    expert_out = lax.map(one_expert, (gate_w, up_w, down_w))
    rows = jnp.arange(tokens.shape[0], dtype=jnp.int32)[:, None]
    chosen = expert_out[routes, rows].astype(jnp.float32)
    return lax.optimization_barrier(jnp.sum(route_weights[:, :, None] * chosen, axis=1)).astype(jnp.bfloat16)
```

```python
import functools

import jax
import jax.numpy as jnp
from jax import lax
from jax.experimental import pallas as pl
from jax.experimental.pallas import tpu as pltpu
from jax.sharding import PartitionSpec as P

MESH = pl.DeviceIdType.MESH
SIDE = 4
CAP = 16
N_Y = 4
BLK = 256


def offset(k, j):
    dz = j // 2
    return dz, 2 * (j % 2) + (k + dz) % 2


def kernel(
    tok_hbm, gain_hbm, bias_hbm, routes_hbm, weights_hbm, gate_hbm, up_hbm, down_hbm,
    out_ref,
    tok, gain, bias, routes, weights, w_in, w_out, swap_in, swap_out,
    out_buf, x_buf, y_buf, r_buf, z_buf, z_own, zr_buf,
    load_sem, wload_sem, swap_send, swap_recv, d_send, d_recv, r_send, r_recv, z_send, z_recv,
):
    ep, tp = lax.axis_index("ep"), lax.axis_index("tp")
    z, x = ep // SIDE, ep % SIDE
    y, c = tp // 2, tp % 2
    k = (z + x + c) % 2
    par = (z + x) % 2

    small = [
        pltpu.make_async_copy(src, dst, load_sem.at[i])
        for i, (src, dst) in enumerate(
            ((tok_hbm, tok), (gain_hbm, gain), (bias_hbm, bias), (routes_hbm, routes), (weights_hbm, weights))
        )
    ]
    for copy in small:
        copy.start()
    big = [
        pltpu.make_async_copy(gate_hbm.at[0], w_in.at[0], wload_sem.at[0]),
        pltpu.make_async_copy(up_hbm.at[0], w_in.at[1], wload_sem.at[1]),
        pltpu.make_async_copy(down_hbm.at[0], w_out, wload_sem.at[2]),
    ]
    for copy in big:
        copy.start()

    barrier = pltpu.get_barrier_semaphore()
    for dz in range(SIDE):
        for dx in range(SIDE):
            for dc in range(2):
                if dz or dx or dc:
                    pl.semaphore_signal(
                        barrier, inc=1,
                        device_id=(((z + dz) % SIDE) * SIDE + (x + dx) % SIDE, y * 2 + (c + dc) % 2),
                        device_id_type=MESH,
                    )
    for dy in range(1, N_Y):
        pl.semaphore_signal(barrier, inc=1, device_id=(ep, ((y + dy) % N_Y) * 2 + c), device_id_type=MESH)

    for copy in small:
        copy.wait()
    rows = tok.shape[0]
    values = tok[...].astype(jnp.float32)
    centred = values - jnp.mean(values, axis=-1, keepdims=True)
    variance = jnp.mean(centred * centred, axis=-1, keepdims=True)
    normed = (centred * lax.rsqrt(variance + 1e-05) * gain[...] + bias[...]).astype(jnp.bfloat16)

    width = 2 * 8 * CAP
    col = lax.broadcasted_iota(jnp.int32, (rows, width), 1)
    dz = (col // (2 * CAP)) % 4
    dx = 2 * ((col // CAP) % 2) + (col // (8 * CAP) + dz) % 2
    expert = ((z + dz) % SIDE) * SIDE + (x + dx) % SIDE
    named = jnp.zeros((rows, width), jnp.float32)
    weight = jnp.zeros((rows, width), jnp.float32)
    for i in range(routes.shape[1]):
        hit = routes[:, i : i + 1] == expert
        named = jnp.where(hit, 1.0, named)
        weight = jnp.where(hit, weights[:, i : i + 1], weight)
    earlier = (
        lax.broadcasted_iota(jnp.int32, (rows, rows), 1) < lax.broadcasted_iota(jnp.int32, (rows, rows), 0)
    ).astype(jnp.float32).astype(jnp.bfloat16)
    rank = jnp.dot(earlier, named.astype(jnp.bfloat16), preferred_element_type=jnp.float32)
    here = (named > 0.5) & (rank == (col % CAP).astype(jnp.float32))
    picker = jnp.where(here, 1.0, 0.0)
    mine = jnp.where(k == 0, picker[:, : width // 2], picker[:, width // 2 :]).astype(jnp.bfloat16)
    outgoing = lax.dot_general(mine, normed, (((0,), (0,)), ((), ())), preferred_element_type=jnp.float32)
    out_buf[...] = outgoing.astype(jnp.bfloat16).reshape(out_buf.shape)

    pl.semaphore_wait(barrier, 2 * SIDE * SIDE - 1 + N_Y - 1)

    sibling = (ep, y * 2 + 1 - c)
    swaps = []
    for i, (src, dst) in enumerate(((w_in.at[0], swap_in.at[0]), (w_in.at[1], swap_in.at[1]), (w_out, swap_out))):
        swaps.append(
            pltpu.make_async_remote_copy(
                src_ref=src, dst_ref=dst, send_sem=swap_send.at[i], recv_sem=swap_recv.at[i],
                device_id=sibling, device_id_type=MESH,
            )
        )

    def dispatch(j):
        dz, dx = offset(k, j)
        return pltpu.make_async_remote_copy(
            src_ref=out_buf.at[j], dst_ref=x_buf.at[j], send_sem=d_send.at[j], recv_sem=d_recv.at[j],
            device_id=(((z + dz) % SIDE) * SIDE + (x + dx) % SIDE, y * 2 + par), device_id_type=MESH,
        )

    order = (5, 4, 1, 2, 3, 6, 7)
    for j in order:
        dispatch(j).start()

    @pl.when(k == 1)
    def _():
        dispatch(0).start()

    @pl.when(k == 0)
    def _():
        x_buf[0] = out_buf[0]

    for load, swap in zip(big, swaps):
        load.wait()
        swap.start()

    for j in order:
        dispatch(j).wait_recv()

    @pl.when(k == 1)
    def _():
        dispatch(0).wait_recv()

    def hidden_of(both):
        rows_in = x_buf[...].reshape(8 * CAP, x_buf.shape[2])
        gate = jnp.dot(rows_in, both[0], preferred_element_type=jnp.float32)
        up = jnp.dot(rows_in, both[1], preferred_element_type=jnp.float32)
        return (gate / (1.0 + jnp.exp(-gate)) * up).astype(jnp.bfloat16)

    hidden_own = hidden_of(w_in)
    swaps[0].wait_recv()
    swaps[1].wait_recv()
    hidden_swap = hidden_of(swap_in)
    swaps[2].wait_recv()

    def give_back(h, j):
        dz, dx = offset(k, j)
        return pltpu.make_async_remote_copy(
            src_ref=y_buf.at[h, j], dst_ref=r_buf.at[k * 8 + j], send_sem=r_send.at[h, j], recv_sem=r_recv.at[k * 8 + j],
            device_id=(((z - dz + SIDE) % SIDE) * SIDE + (x - dx + SIDE) % SIDE, y * 2 + h), device_id_type=MESH,
        )

    for h in range(2):
        for part in range(N_Y):
            cols = pl.ds((2 * part + h) * BLK, BLK)
            piece = jnp.dot(hidden_own, w_out[:, cols], preferred_element_type=jnp.float32)
            piece += jnp.dot(hidden_swap, swap_out[:, cols], preferred_element_type=jnp.float32)
            y_buf[h, :, :, part * BLK : (part + 1) * BLK] = piece.astype(jnp.bfloat16).reshape(8, CAP, BLK)
        for j in order:
            give_back(h, j).start()
        local = (k == 0) & (c == h)

        @pl.when(local)
        def _():
            r_buf[0] = y_buf[h, 0]

        @pl.when(jnp.logical_not(local))
        def _():
            give_back(h, 0).start()

    def arrival(i):
        return pltpu.make_async_remote_copy(
            src_ref=y_buf.at[0, 0], dst_ref=r_buf.at[i], send_sem=r_send.at[0, 0], recv_sem=r_recv.at[i],
            device_id=sibling, device_id_type=MESH,
        )

    for i in range(1, 16):
        arrival(i).wait_recv()

    @pl.when(k == 1)
    def _():
        arrival(0).wait_recv()

    scaled = jnp.where(here, weight, 0.0)
    high = scaled.astype(jnp.bfloat16)
    low = (scaled - high.astype(jnp.float32)).astype(jnp.bfloat16)
    both = jnp.concatenate([high, low], axis=0)
    for part in range(N_Y):
        got = r_buf[:, :, part * BLK : (part + 1) * BLK].reshape(16 * CAP, BLK)
        twice = jnp.dot(both, got, preferred_element_type=jnp.float32)
        summed = twice[:rows] + twice[rows:]
        z_own[part] = summed
        z_buf[part] = summed.astype(jnp.bfloat16)

    def across(i):
        there = (y + i) % N_Y
        return pltpu.make_async_remote_copy(
            src_ref=z_buf.at[there], dst_ref=zr_buf.at[i - 1], send_sem=z_send.at[i - 1], recv_sem=z_recv.at[i - 1],
            device_id=(ep, there * 2 + c), device_id_type=MESH,
        )

    for i in (2, 1, 3):
        across(i).start()
    total = z_own[y]
    for i in (1, 3, 2):
        across(i).wait_recv()
    for i in range(3):
        total += zr_buf[i].astype(jnp.float32)
    out_ref[...] = total.astype(out_ref.dtype)

    for swap in swaps:
        swap.wait_send()
    for j in order:
        dispatch(j).wait_send()

    @pl.when(k == 1)
    def _():
        dispatch(0).wait_send()

    for h in range(2):
        for j in order:
            give_back(h, j).wait_send()

        @pl.when(jnp.logical_not((k == 0) & (c == h)))
        def _():
            give_back(h, 0).wait_send()
    for i in range(1, N_Y):
        across(i).wait_send()


def body(tokens, norm_gain, norm_bias, routes, route_weights, gate_w, up_w, down_w):
    rows, width = tokens.shape
    half = gate_w.shape[2]
    any_ = pl.BlockSpec(memory_space=pl.ANY)
    bf16, f32 = jnp.bfloat16, jnp.float32
    dma = pltpu.SemaphoreType.DMA
    return pl.pallas_call(
        kernel,
        name="moe",
        out_shape=jax.ShapeDtypeStruct((rows, BLK), bf16),
        in_specs=[any_] * 8,
        out_specs=pl.BlockSpec(memory_space=pltpu.VMEM),
        scratch_shapes=[
            pltpu.VMEM((rows, width), bf16),
            pltpu.VMEM((1, width), f32),
            pltpu.VMEM((1, width), f32),
            pltpu.VMEM(routes.shape, jnp.int32),
            pltpu.VMEM(route_weights.shape, f32),
            pltpu.VMEM((2, width, half), bf16),
            pltpu.VMEM((half, width), bf16),
            pltpu.VMEM((2, width, half), bf16),
            pltpu.VMEM((half, width), bf16),
            pltpu.VMEM((8, CAP, width), bf16),
            pltpu.VMEM((8, CAP, width), bf16),
            pltpu.VMEM((2, 8, CAP, width // 2), bf16),
            pltpu.VMEM((16, CAP, width // 2), bf16),
            pltpu.VMEM((N_Y, rows, BLK), bf16),
            pltpu.VMEM((N_Y, rows, BLK), f32),
            pltpu.VMEM((N_Y - 1, rows, BLK), bf16),
            dma((5,)), dma((3,)), dma((3,)), dma((3,)), dma((8,)), dma((8,)), dma((2, 8)), dma((16,)), dma((3,)), dma((3,)),
        ],
        compiler_params=pltpu.CompilerParams(collective_id=0, has_side_effects=True),
    )(
        tokens, norm_gain.reshape(1, width), norm_bias.reshape(1, width), routes, route_weights, gate_w, up_w, down_w
    )


def solution(mesh):
    placed = (
        P("ep", None),
        P(),
        P(),
        P("ep", None),
        P("ep", None),
        P("ep", None, "tp"),
        P("ep", None, "tp"),
        P("ep", "tp", None),
    )
    return jax.shard_map(body, mesh=mesh, in_specs=placed, out_specs=P("ep", "tp"), check_vma=False)
```

```python
import jax
import jax.numpy as jnp
from jax import lax
from jax.experimental import pallas as pl
from jax.experimental.pallas import tpu as pltpu
from jax.sharding import PartitionSpec as P

MESH = pl.DeviceIdType.MESH
SIDE = 4
CAP = 16
BLK = 256
CHUNKS = 1
OFFSETS = (
    ((2, 2), (1, 1), (3, 3), (1, 3), (3, 1), (0, 2), (2, 0), (0, 0)),
    ((1, 2), (2, 1), (3, 2), (2, 3), (0, 1), (0, 3), (1, 0), (3, 0)),
)


def offset(k, i):
    (z0, x0), (z1, x1) = OFFSETS[0][i], OFFSETS[1][i]
    return z0 + k * (z1 - z0), x0 + k * (x1 - x0)


def packed(which):
    word = 0
    for n, pair in enumerate(OFFSETS[1] + OFFSETS[0]):
        word |= pair[which] << (2 * n)
    return word - (1 << 32) if word >= 1 << 31 else word


def kernel(
    tok_hbm, gain_hbm, bias_hbm, routes_hbm, weights_hbm, gate_hbm, up_hbm, down_hbm,
    out_ref,
    tok, gain, bias, routes, weights, w_in, w_out, swap_in, swap_out,
    out_buf, x_buf, y_buf, r_buf,
    load_sem, wload_sem, swap_send, swap_recv, d_send, d_recv, r_send, r_recv, plane_sem,
):
    ep, tp = lax.axis_index("ep"), lax.axis_index("tp")
    z, x = ep // SIDE, ep % SIDE
    y, c = tp // 2, tp % 2
    par = (z + x) % 2
    k = (par + c) % 2

    def chip(dz, dx):
        return ((z + dz) % SIDE) * SIDE + (x + dx) % SIDE

    small = [
        pltpu.make_async_copy(src, dst, load_sem.at[i])
        for i, (src, dst) in enumerate(
            ((tok_hbm, tok), (gain_hbm, gain), (bias_hbm, bias), (routes_hbm, routes), (weights_hbm, weights))
        )
    ]
    for copy in small:
        copy.start()
    big = [
        pltpu.make_async_copy(gate_hbm.at[0], w_in.at[0], wload_sem.at[0]),
        pltpu.make_async_copy(up_hbm.at[0], w_in.at[1], wload_sem.at[1]),
        pltpu.make_async_copy(down_hbm.at[0], w_out, wload_sem.at[2]),
    ]
    for copy in big:
        copy.start()

    barrier = pltpu.get_barrier_semaphore()
    for dz in range(SIDE):
        for dx in range(SIDE):
            for dc in range(2):
                if dz or dx or dc:
                    pl.semaphore_signal(
                        barrier, inc=1, device_id=(chip(dz, dx), y * 2 + (c + dc) % 2), device_id_type=MESH
                    )
    column = [(ep, ((y + dy) % SIDE) * 2 + c) for dy in range(1, SIDE)]
    for there in column:
        pl.semaphore_signal(barrier, inc=1, device_id=there, device_id_type=MESH)

    for copy in small:
        copy.wait()
    rows = tok.shape[0]
    values = tok[...].astype(jnp.float32)
    centred = values - jnp.mean(values, axis=-1, keepdims=True)
    variance = jnp.mean(centred * centred, axis=-1, keepdims=True)
    normed = (centred * lax.rsqrt(variance + 1e-05) * gain[...] + bias[...]).astype(jnp.bfloat16)

    slots = 16 * CAP
    slot = lax.broadcasted_iota(jnp.int32, (slots, rows), 0)
    shift = 2 * (slot // CAP)
    dz = lax.shift_right_logical(jnp.full_like(slot, packed(0)), shift) & 3
    dx = lax.shift_right_logical(jnp.full_like(slot, packed(1)), shift) & 3
    expert = ((z + dz) & 3) * SIDE + ((x + dx) & 3)
    named = jnp.zeros((slots, rows), jnp.float32)
    weight = jnp.zeros((slots, rows), jnp.float32)
    for i in range(routes.shape[0]):
        hit = routes[i : i + 1, :] == expert
        named = jnp.where(hit, 1.0, named)
        weight = jnp.where(hit, weights[i : i + 1, :], weight)
    earlier = (
        lax.broadcasted_iota(jnp.int32, (rows, rows), 0) < lax.broadcasted_iota(jnp.int32, (rows, rows), 1)
    ).astype(jnp.float32).astype(jnp.bfloat16)
    rank = jnp.dot(named.astype(jnp.bfloat16), earlier, preferred_element_type=jnp.float32)
    here = (named > 0.5) & (rank == (slot % CAP).astype(jnp.float32))
    picker = jnp.where(here, 1.0, 0.0)
    mine = jnp.where(k == 1, picker[: slots // 2], picker[slots // 2 :]).astype(jnp.bfloat16)
    outgoing = jnp.dot(mine, normed, preferred_element_type=jnp.float32)
    out_buf[...] = outgoing.astype(jnp.bfloat16).reshape(out_buf.shape)

    pl.semaphore_wait(barrier, 2 * SIDE * SIDE - 1 + SIDE - 1)

    sibling = (ep, y * 2 + 1 - c)
    swaps = []
    for i, (src, dst) in enumerate(((w_in.at[0], swap_in.at[0]), (w_in.at[1], swap_in.at[1]), (w_out, swap_out))):
        swaps.append(
            pltpu.make_async_remote_copy(
                src_ref=src, dst_ref=dst, send_sem=swap_send.at[i], recv_sem=swap_recv.at[i],
                device_id=sibling, device_id_type=MESH,
            )
        )

    def dispatch(i):
        dz, dx = offset(k, i)
        return pltpu.make_async_remote_copy(
            src_ref=out_buf.at[i], dst_ref=x_buf.at[i], send_sem=d_send.at[i], recv_sem=d_recv.at[i],
            device_id=(chip(dz, dx), y * 2 + par), device_id_type=MESH,
        )

    for i in range(7):
        dispatch(i).start()

    @pl.when(k == 1)
    def _():
        dispatch(7).start()

    @pl.when(k == 0)
    def _():
        x_buf[7] = out_buf[7]

    for there in column:
        pl.semaphore_signal(plane_sem, inc=1, device_id=there, device_id_type=MESH)

    for load, swap in zip(big, swaps):
        load.wait()
        swap.start()

    def hidden_of(rows_in, both):
        gate = jnp.dot(rows_in, both[0], preferred_element_type=jnp.float32)
        up = jnp.dot(rows_in, both[1], preferred_element_type=jnp.float32)
        return (gate / (1.0 + jnp.exp(-gate)) * up).astype(jnp.bfloat16)

    def give_back(i, dy, h):
        dz, dx = offset(k, i)
        own = i == 7 and dy == 0
        return pltpu.make_async_remote_copy(
            src_ref=y_buf.at[i, dy, h], dst_ref=r_buf.at[dy, (1 - k) * 8 + i],
            send_sem=r_send.at[h + 1 if own else 0 if i < 7 else 3],
            recv_sem=r_recv.at[4 * (1 - k) if own else dy],
            device_id=(chip(SIDE - dz, SIDE - dx), ((y + dy) % SIDE) * 2 + h), device_id_type=MESH,
        )

    per = 8 // CHUNKS
    for chunk in range(CHUNKS):
        first = chunk * per
        for i in range(first, first + per):
            if i < 7:
                dispatch(i).wait_recv()
            else:

                @pl.when(k == 1)
                def _():
                    dispatch(7).wait_recv()

        rows_in = x_buf[first : first + per].reshape(per * CAP, x_buf.shape[2])
        hidden_own = hidden_of(rows_in, w_in)
        if chunk == 0:
            swaps[0].wait_recv()
            swaps[1].wait_recv()
        hidden_swap = hidden_of(rows_in, swap_in)
        if chunk == 0:
            swaps[2].wait_recv()
            pl.semaphore_wait(plane_sem, SIDE - 1)
        for dy in (2, 1, 3, 0):
            for h in range(2):
                cols = pl.ds(pl.multiple_of((((y + dy) % SIDE) * 2 + h) * BLK, BLK), BLK)
                piece = jnp.dot(hidden_own, w_out[:, cols], preferred_element_type=jnp.float32)
                piece += jnp.dot(hidden_swap, swap_out[:, cols], preferred_element_type=jnp.float32)
                y_buf[first : first + per, dy, h] = piece.astype(jnp.bfloat16).reshape(per, CAP, BLK)
            for i in range(first, first + per):
                for h in range(2):
                    if i < 7 or dy:
                        give_back(i, dy, h).start()
                    else:
                        local = (k == 0) & (c == h)

                        @pl.when(local)
                        def _():
                            r_buf[0, 15] = y_buf[7, 0, h]

                        @pl.when(jnp.logical_not(local))
                        def _():
                            give_back(7, 0, h).start()

    scaled = jnp.where(here, weight, 0.0).T
    high = scaled.astype(jnp.bfloat16)
    low = (scaled - high.astype(jnp.float32)).astype(jnp.bfloat16)
    both = jnp.concatenate([high, low], axis=0)

    def arrived(blocks, sem):
        return pltpu.make_async_remote_copy(
            src_ref=blocks, dst_ref=blocks, send_sem=r_send.at[0], recv_sem=r_recv.at[sem],
            device_id=sibling, device_id_type=MESH,
        )

    arrived(r_buf.at[0, 0:15], 0).wait_recv()

    @pl.when(k == 1)
    def _():
        arrived(r_buf.at[0, 15], 4).wait_recv()

    for dy in (1, 3, 2):
        arrived(r_buf.at[dy], dy).wait_recv()
    twice = jnp.zeros((2 * rows, BLK), jnp.float32)
    for dy in range(SIDE):
        twice += jnp.dot(both, r_buf[dy].reshape(slots, BLK), preferred_element_type=jnp.float32)
    out_ref[...] = (twice[:rows] + twice[rows:]).astype(out_ref.dtype)

    for swap in swaps:
        swap.wait_send()
    for i in range(7):
        dispatch(i).wait_send()

    @pl.when(k == 1)
    def _():
        dispatch(7).wait_send()

    def sent(blocks, sem):
        return pltpu.make_async_remote_copy(
            src_ref=blocks, dst_ref=blocks, send_sem=r_send.at[sem], recv_sem=r_recv.at[0],
            device_id=sibling, device_id_type=MESH,
        )

    sent(y_buf.at[0:7], 0).wait_send()
    sent(y_buf.at[7, 1:4], 3).wait_send()
    for h in range(2):

        @pl.when(jnp.logical_not((k == 0) & (c == h)))
        def _():
            sent(y_buf.at[7, 0, h], h + 1).wait_send()


def body(tokens, norm_gain, norm_bias, routes, route_weights, gate_w, up_w, down_w):
    rows, width = tokens.shape
    half = gate_w.shape[2]
    hbm = pl.BlockSpec(memory_space=pl.ANY)
    bf16, f32 = jnp.bfloat16, jnp.float32
    dma = pltpu.SemaphoreType.DMA
    return pl.pallas_call(
        kernel,
        name="moe",
        out_shape=jax.ShapeDtypeStruct((rows, BLK), bf16),
        in_specs=[hbm] * 8,
        out_specs=pl.BlockSpec(memory_space=pltpu.VMEM),
        scratch_shapes=[
            pltpu.VMEM((rows, width), bf16),
            pltpu.VMEM((1, width), f32),
            pltpu.VMEM((1, width), f32),
            pltpu.VMEM(routes.shape[::-1], jnp.int32),
            pltpu.VMEM(route_weights.shape[::-1], f32),
            pltpu.VMEM((2, width, half), bf16),
            pltpu.VMEM((half, width), bf16),
            pltpu.VMEM((2, width, half), bf16),
            pltpu.VMEM((half, width), bf16),
            pltpu.VMEM((8, CAP, width), bf16),
            pltpu.VMEM((8, CAP, width), bf16),
            pltpu.VMEM((8, SIDE, 2, CAP, BLK), bf16),
            pltpu.VMEM((SIDE, 16, CAP, BLK), bf16),
            dma((5,)), dma((3,)), dma((3,)), dma((3,)), dma((8,)), dma((8,)), dma((4,)), dma((5,)),
            pltpu.SemaphoreType.REGULAR,
        ],
        compiler_params=pltpu.CompilerParams(collective_id=0, has_side_effects=True),
    )(
        tokens, norm_gain.reshape(1, width), norm_bias.reshape(1, width), routes.T, route_weights.T, gate_w, up_w, down_w
    )


def solution(mesh):
    placed = (
        P("ep", None),
        P(),
        P(),
        P("ep", None),
        P("ep", None),
        P("ep", None, "tp"),
        P("ep", None, "tp"),
        P("ep", "tp", None),
    )
    return jax.shard_map(body, mesh=mesh, in_specs=placed, out_specs=P("ep", "tp"), check_vma=False)
```

```python
import jax
import jax.numpy as jnp
from jax import lax
from jax.experimental import pallas as pl
from jax.experimental.pallas import tpu as pltpu
from jax.sharding import PartitionSpec as P

MESH = pl.DeviceIdType.MESH
SIDE = 4
CAP = 16
BLK = 256
CHUNKS = 2
OFFSETS = (
    ((2, 2), (1, 1), (3, 3), (1, 3), (3, 1), (0, 2), (2, 0), (0, 0)),
    ((1, 2), (2, 1), (3, 2), (2, 3), (0, 1), (0, 3), (1, 0), (3, 0)),
)


def offset(k, i):
    (z0, x0), (z1, x1) = OFFSETS[0][i], OFFSETS[1][i]
    return z0 + k * (z1 - z0), x0 + k * (x1 - x0)


def packed(which):
    word = 0
    for n, pair in enumerate(OFFSETS[1] + OFFSETS[0]):
        word |= pair[which] << (2 * n)
    return word - (1 << 32) if word >= 1 << 31 else word


def kernel(
    tok_hbm, gain_hbm, bias_hbm, routes_hbm, weights_hbm, gate_hbm, up_hbm, down_hbm,
    out_ref,
    tok, gain, bias, routes, weights, w_in, w_out, swap_in, swap_out,
    out_buf, x_buf, y_buf, r_buf,
    load_sem, wload_sem, swap_send, swap_recv, d_send, d_recv, r_send, r_recv, near_sem, plane_sem,
):
    ep, tp = lax.axis_index("ep"), lax.axis_index("tp")
    z, x = ep // SIDE, ep % SIDE
    y, c = tp // 2, tp % 2
    par = (z + x) % 2
    k = (par + c) % 2

    def chip(dz, dx):
        return ((z + dz) % SIDE) * SIDE + (x + dx) % SIDE

    sibling = (ep, y * 2 + 1 - c)
    barrier = pltpu.get_barrier_semaphore()

    @pl.when(c == 1)
    def _():
        pl.semaphore_signal(barrier, inc=1, device_id=sibling, device_id_type=MESH)

    for dz in range(SIDE):
        for dx in range(SIDE):
            if dz or dx:
                pl.semaphore_signal(barrier, inc=1, device_id=(chip(dz, dx), y * 2 + 1), device_id_type=MESH)
    for dy in range(1, SIDE):
        pl.semaphore_signal(barrier, inc=1, device_id=(ep, ((y + dy) % SIDE) * 2 + 1), device_id_type=MESH)

    small = [
        pltpu.make_async_copy(src, dst, load_sem.at[i])
        for i, (src, dst) in enumerate(
            ((tok_hbm, tok), (gain_hbm, gain), (bias_hbm, bias), (routes_hbm, routes), (weights_hbm, weights))
        )
    ]
    for copy in small:
        copy.start()
    big = [
        pltpu.make_async_copy(gate_hbm.at[0], w_in.at[0], wload_sem.at[0]),
        pltpu.make_async_copy(up_hbm.at[0], w_in.at[1], wload_sem.at[1]),
        pltpu.make_async_copy(down_hbm.at[0], w_out, wload_sem.at[2]),
    ]
    for copy in big:
        copy.start()

    @pl.when(c == 0)
    def _():
        pl.semaphore_wait(barrier, 1)
        pl.semaphore_signal(near_sem, inc=1, device_id=sibling, device_id_type=MESH)

    @pl.when(c == 1)
    def _():
        pl.semaphore_wait(near_sem, 1)

    swaps = []
    for i, (src, dst) in enumerate(
        ((gate_hbm.at[0], swap_in.at[0]), (up_hbm.at[0], swap_in.at[1]), (down_hbm.at[0], swap_out))
    ):
        swaps.append(
            pltpu.make_async_remote_copy(
                src_ref=src, dst_ref=dst, send_sem=swap_send.at[i], recv_sem=swap_recv.at[i],
                device_id=sibling, device_id_type=MESH,
            )
        )
        swaps[-1].start()

    for copy in small:
        copy.wait()
    rows = tok.shape[0]
    values = tok[...].astype(jnp.float32)
    centred = values - jnp.mean(values, axis=-1, keepdims=True)
    variance = jnp.mean(centred * centred, axis=-1, keepdims=True)
    normed = (centred * lax.rsqrt(variance + 1e-05) * gain[...] + bias[...]).astype(jnp.bfloat16)

    slots = 16 * CAP
    slot = lax.broadcasted_iota(jnp.int32, (slots, rows), 0)
    shift = 2 * (slot // CAP)
    dz = lax.shift_right_logical(jnp.full_like(slot, packed(0)), shift) & 3
    dx = lax.shift_right_logical(jnp.full_like(slot, packed(1)), shift) & 3
    expert = ((z + dz) & 3) * SIDE + ((x + dx) & 3)
    named = jnp.zeros((slots, rows), jnp.float32)
    weight = jnp.zeros((slots, rows), jnp.float32)
    for i in range(routes.shape[0]):
        hit = routes[i : i + 1, :] == expert
        named = jnp.where(hit, 1.0, named)
        weight = jnp.where(hit, weights[i : i + 1, :], weight)
    earlier = (
        lax.broadcasted_iota(jnp.int32, (rows, rows), 0) < lax.broadcasted_iota(jnp.int32, (rows, rows), 1)
    ).astype(jnp.float32).astype(jnp.bfloat16)
    rank = jnp.dot(named.astype(jnp.bfloat16), earlier, preferred_element_type=jnp.float32)
    here = (named > 0.5) & (rank == (slot % CAP).astype(jnp.float32))
    picker = jnp.where(here, 1.0, 0.0)
    mine = jnp.where(k == 1, picker[: slots // 2], picker[slots // 2 :]).astype(jnp.bfloat16)
    outgoing = jnp.dot(mine, normed, preferred_element_type=jnp.float32)
    out_buf[...] = outgoing.astype(jnp.bfloat16).reshape(out_buf.shape)

    @pl.when(c == 1)
    def _():
        pl.semaphore_wait(barrier, 2 * (SIDE * SIDE - 1 + SIDE - 1))
        pl.semaphore_signal(near_sem, inc=1, device_id=sibling, device_id_type=MESH)

    @pl.when(c == 0)
    def _():
        pl.semaphore_wait(near_sem, 1)

    def dispatch(i):
        dz, dx = offset(k, i)
        return pltpu.make_async_remote_copy(
            src_ref=out_buf.at[i], dst_ref=x_buf.at[i], send_sem=d_send.at[i], recv_sem=d_recv.at[i],
            device_id=(chip(dz, dx), y * 2 + par), device_id_type=MESH,
        )

    for i in range(7):
        dispatch(i).start()

    @pl.when(k == 1)
    def _():
        dispatch(7).start()

    @pl.when(k == 0)
    def _():
        x_buf[7] = out_buf[7]

    @pl.when(c == 1)
    def _():
        for dy in range(1, SIDE):
            for core in range(2):
                there = (ep, ((y + dy) % SIDE) * 2 + core)
                pl.semaphore_signal(plane_sem, inc=1, device_id=there, device_id_type=MESH)

    for copy in big:
        copy.wait()

    def hidden_of(rows_in, both):
        gate = jnp.dot(rows_in, both[0], preferred_element_type=jnp.float32)
        up = jnp.dot(rows_in, both[1], preferred_element_type=jnp.float32)
        return (gate / (1.0 + jnp.exp(-gate)) * up).astype(jnp.bfloat16)

    def give_back(i, dy, h):
        dz, dx = offset(k, i)
        own = i == 7 and dy == 0
        return pltpu.make_async_remote_copy(
            src_ref=y_buf.at[i, dy, h], dst_ref=r_buf.at[dy, (1 - k) * 8 + i],
            send_sem=r_send.at[h + 1 if own else 0 if i < 7 else 3],
            recv_sem=r_recv.at[4 * (1 - k) if own else dy],
            device_id=(chip(SIDE - dz, SIDE - dx), ((y + dy) % SIDE) * 2 + h), device_id_type=MESH,
        )

    per = 8 // CHUNKS
    for chunk in range(CHUNKS):
        first = chunk * per
        for i in range(first, first + per):
            if i < 7:
                dispatch(i).wait_recv()
            else:

                @pl.when(k == 1)
                def _():
                    dispatch(7).wait_recv()

        rows_in = x_buf[first : first + per].reshape(per * CAP, x_buf.shape[2])
        hidden_own = hidden_of(rows_in, w_in)
        if chunk == 0:
            swaps[0].wait_recv()
            swaps[1].wait_recv()
        hidden_swap = hidden_of(rows_in, swap_in)
        if chunk == 0:
            swaps[2].wait_recv()
            pl.semaphore_wait(plane_sem, SIDE - 1)
        for dy in (2, 1, 3, 0):
            for h in range(2):
                cols = pl.ds(pl.multiple_of((((y + dy) % SIDE) * 2 + h) * BLK, BLK), BLK)
                piece = jnp.dot(hidden_own, w_out[:, cols], preferred_element_type=jnp.float32)
                piece += jnp.dot(hidden_swap, swap_out[:, cols], preferred_element_type=jnp.float32)
                y_buf[first : first + per, dy, h] = piece.astype(jnp.bfloat16).reshape(per, CAP, BLK)
            for i in range(first, first + per):
                for h in range(2):
                    if i < 7 or dy:
                        give_back(i, dy, h).start()
                    else:
                        local = (k == 0) & (c == h)

                        @pl.when(local)
                        def _():
                            r_buf[0, 15] = y_buf[7, 0, h]

                        @pl.when(jnp.logical_not(local))
                        def _():
                            give_back(7, 0, h).start()

    scaled = jnp.where(here, weight, 0.0).T
    high = scaled.astype(jnp.bfloat16)
    low = (scaled - high.astype(jnp.float32)).astype(jnp.bfloat16)
    both = jnp.concatenate([high, low], axis=0)

    def arrived(blocks, sem):
        return pltpu.make_async_remote_copy(
            src_ref=blocks, dst_ref=blocks, send_sem=r_send.at[0], recv_sem=r_recv.at[sem],
            device_id=sibling, device_id_type=MESH,
        )

    arrived(r_buf.at[0, 0:15], 0).wait_recv()

    @pl.when(k == 1)
    def _():
        arrived(r_buf.at[0, 15], 4).wait_recv()

    for dy in (1, 3, 2):
        arrived(r_buf.at[dy], dy).wait_recv()
    twice = jnp.zeros((2 * rows, BLK), jnp.float32)
    for dy in range(SIDE):
        twice += jnp.dot(both, r_buf[dy].reshape(slots, BLK), preferred_element_type=jnp.float32)
    out_ref[...] = (twice[:rows] + twice[rows:]).astype(out_ref.dtype)

    for swap in swaps:
        swap.wait_send()
    for i in range(7):
        dispatch(i).wait_send()

    @pl.when(k == 1)
    def _():
        dispatch(7).wait_send()

    def sent(blocks, sem):
        return pltpu.make_async_remote_copy(
            src_ref=blocks, dst_ref=blocks, send_sem=r_send.at[sem], recv_sem=r_recv.at[0],
            device_id=sibling, device_id_type=MESH,
        )

    sent(y_buf.at[0:7], 0).wait_send()
    sent(y_buf.at[7, 1:4], 3).wait_send()
    for h in range(2):

        @pl.when(jnp.logical_not((k == 0) & (c == h)))
        def _():
            sent(y_buf.at[7, 0, h], h + 1).wait_send()


def body(tokens, norm_gain, norm_bias, routes, route_weights, gate_w, up_w, down_w):
    rows, width = tokens.shape
    half = gate_w.shape[2]
    hbm = pl.BlockSpec(memory_space=pltpu.HBM)
    bf16, f32 = jnp.bfloat16, jnp.float32
    dma = pltpu.SemaphoreType.DMA
    return pl.pallas_call(
        kernel,
        name="moe",
        out_shape=pltpu.VMEM((rows, BLK), bf16),
        in_specs=[hbm] * 8,
        out_specs=pl.BlockSpec(memory_space=pltpu.VMEM),
        scratch_shapes=[
            pltpu.VMEM((rows, width), bf16),
            pltpu.VMEM((1, width), f32),
            pltpu.VMEM((1, width), f32),
            pltpu.VMEM(routes.shape[::-1], jnp.int32),
            pltpu.VMEM(route_weights.shape[::-1], f32),
            pltpu.VMEM((2, width, half), bf16),
            pltpu.VMEM((half, width), bf16),
            pltpu.VMEM((2, width, half), bf16),
            pltpu.VMEM((half, width), bf16),
            pltpu.VMEM((8, CAP, width), bf16),
            pltpu.VMEM((8, CAP, width), bf16),
            pltpu.VMEM((8, SIDE, 2, CAP, BLK), bf16),
            pltpu.VMEM((SIDE, 16, CAP, BLK), bf16),
            dma((5,)), dma((3,)), dma((3,)), dma((3,)), dma((8,)), dma((8,)), dma((4,)), dma((5,)),
            pltpu.SemaphoreType.REGULAR,
            pltpu.SemaphoreType.REGULAR,
        ],
        compiler_params=pltpu.CompilerParams(collective_id=0, has_side_effects=True, vmem_limit_bytes=32 << 20),
    )(
        *(
            pltpu.with_memory_space_constraint(a, pltpu.HBM)
            for a in (
                tokens, norm_gain.reshape(1, width), norm_bias.reshape(1, width), routes.T, route_weights.T, gate_w, up_w, down_w
            )
        )
    )


def solution(mesh):
    placed = (
        P("ep", None),
        P(),
        P(),
        P("ep", None),
        P("ep", None),
        P("ep", None, "tp"),
        P("ep", None, "tp"),
        P("ep", "tp", None),
    )
    return jax.shard_map(body, mesh=mesh, in_specs=placed, out_specs=P("ep", "tp"), check_vma=False)
```

```python
import jax
import jax.numpy as jnp
from jax import lax
from jax.experimental import pallas as pl
from jax.experimental.pallas import tpu as pltpu
from jax.sharding import PartitionSpec as P

MESH = pl.DeviceIdType.MESH
SIDE = 4
CAP = 16
BLK = 256
CHUNKS = ((0, 1, 2, 7), (3, 4, 5, 6))
ORDER = (0, 1, 2, 7, 3, 4, 5, 6)
OFFSETS = (
    ((2, 2), (1, 1), (3, 3), (1, 3), (3, 1), (0, 2), (2, 0), (0, 0)),
    ((1, 2), (3, 2), (1, 0), (2, 1), (2, 3), (0, 1), (0, 3), (3, 0)),
)


GROUPS = ((1,), (3,), (2,), (0,))


def sending(group, members):
    return [(dy, i, h) for dy in group for i in members for h in range(2)]


def offset(k, i):
    (z0, x0), (z1, x1) = OFFSETS[0][i], OFFSETS[1][i]
    return z0 + k * (z1 - z0), x0 + k * (x1 - x0)


def packed(which):
    word = 0
    for n, pair in enumerate(OFFSETS[1] + OFFSETS[0]):
        word |= pair[which] << (2 * n)
    return word - (1 << 32) if word >= 1 << 31 else word


def kernel(
    tok_hbm, gain_hbm, bias_hbm, routes_hbm, weights_hbm, gate_hbm, up_hbm, down_hbm,
    out_ref,
    tok, gain, bias, routes, weights, w_in, w_out, swap_in, swap_out,
    out_buf, x_buf, y_buf, r_buf,
    load_sem, wload_sem, swap_send, swap_recv, d_send, d_recv, r_send, r_recv, near_sem, plane_sem,
):
    ep, tp = lax.axis_index("ep"), lax.axis_index("tp")
    z, x = ep // SIDE, ep % SIDE
    y, c = tp // 2, tp % 2
    par = (z + x) % 2
    k = (par + c) % 2

    def chip(dz, dx):
        return ((z + dz) % SIDE) * SIDE + (x + dx) % SIDE

    sibling = (ep, y * 2 + 1 - c)
    barrier = pltpu.get_barrier_semaphore()

    @pl.when(c == 1)
    def _():
        pl.semaphore_signal(barrier, inc=1, device_id=sibling, device_id_type=MESH)

    for dz in range(SIDE):
        for dx in range(SIDE):
            if dz or dx:
                pl.semaphore_signal(barrier, inc=1, device_id=(chip(dz, dx), y * 2 + 1), device_id_type=MESH)
    for dy in range(1, SIDE):
        pl.semaphore_signal(barrier, inc=1, device_id=(ep, ((y + dy) % SIDE) * 2 + 1), device_id_type=MESH)

    small = [
        pltpu.make_async_copy(src, dst, load_sem.at[i])
        for i, (src, dst) in enumerate(
            ((tok_hbm, tok), (gain_hbm, gain), (bias_hbm, bias), (routes_hbm, routes), (weights_hbm, weights))
        )
    ]
    for copy in small:
        copy.start()
    big = [
        pltpu.make_async_copy(gate_hbm.at[0], w_in.at[0], wload_sem.at[0]),
        pltpu.make_async_copy(up_hbm.at[0], w_in.at[1], wload_sem.at[1]),
        pltpu.make_async_copy(down_hbm.at[0], w_out, wload_sem.at[2]),
    ]
    for copy in big:
        copy.start()

    @pl.when(c == 0)
    def _():
        pl.semaphore_wait(barrier, 1)
        pl.semaphore_signal(near_sem, inc=1, device_id=sibling, device_id_type=MESH)

    @pl.when(c == 1)
    def _():
        pl.semaphore_wait(near_sem, 1)

    swaps = []
    for i, (src, dst) in enumerate(
        ((gate_hbm.at[0], swap_in.at[0]), (up_hbm.at[0], swap_in.at[1]), (down_hbm.at[0], swap_out))
    ):
        swaps.append(
            pltpu.make_async_remote_copy(
                src_ref=src, dst_ref=dst, send_sem=swap_send.at[i], recv_sem=swap_recv.at[i],
                device_id=sibling, device_id_type=MESH,
            )
        )
        swaps[-1].start()

    for copy in small:
        copy.wait()
    rows = tok.shape[0]
    values = tok[...].astype(jnp.float32)
    centred = values - jnp.mean(values, axis=-1, keepdims=True)
    variance = jnp.mean(centred * centred, axis=-1, keepdims=True)
    normed = (centred * lax.rsqrt(variance + 1e-05) * gain[...] + bias[...]).astype(jnp.bfloat16)

    slots = 16 * CAP
    slot = lax.broadcasted_iota(jnp.int32, (slots, rows), 0)
    shift = 2 * (slot // CAP)
    dz = lax.shift_right_logical(jnp.full_like(slot, packed(0)), shift) & 3
    dx = lax.shift_right_logical(jnp.full_like(slot, packed(1)), shift) & 3
    expert = ((z + dz) & 3) * SIDE + ((x + dx) & 3)
    named = jnp.zeros((slots, rows), jnp.float32)
    weight = jnp.zeros((slots, rows), jnp.float32)
    for i in range(routes.shape[0]):
        hit = routes[i : i + 1, :] == expert
        named = jnp.where(hit, 1.0, named)
        weight = jnp.where(hit, weights[i : i + 1, :], weight)
    earlier = (
        lax.broadcasted_iota(jnp.int32, (rows, rows), 0) < lax.broadcasted_iota(jnp.int32, (rows, rows), 1)
    ).astype(jnp.float32).astype(jnp.bfloat16)
    rank = jnp.dot(named.astype(jnp.bfloat16), earlier, preferred_element_type=jnp.float32)
    here = (named > 0.5) & (rank == (slot % CAP).astype(jnp.float32))
    picker = jnp.where(here, 1.0, 0.0)
    mine = jnp.where(k == 1, picker[: slots // 2], picker[slots // 2 :]).astype(jnp.bfloat16)
    outgoing = jnp.dot(mine, normed, preferred_element_type=jnp.float32)
    out_buf[...] = outgoing.astype(jnp.bfloat16).reshape(out_buf.shape)

    @pl.when(c == 1)
    def _():
        pl.semaphore_wait(barrier, 2 * (SIDE * SIDE - 1 + SIDE - 1))
        pl.semaphore_signal(near_sem, inc=1, device_id=sibling, device_id_type=MESH)

    @pl.when(c == 0)
    def _():
        pl.semaphore_wait(near_sem, 1)

    def dispatch(i):
        dz, dx = offset(k, i)
        return pltpu.make_async_remote_copy(
            src_ref=out_buf.at[i], dst_ref=x_buf.at[i], send_sem=d_send.at[i], recv_sem=d_recv.at[i],
            device_id=(chip(dz, dx), y * 2 + par), device_id_type=MESH,
        )

    for i in ORDER:
        if i == CHUNKS[1][0]:
            for n in CHUNKS[0]:
                if n < 7:
                    dispatch(n).wait_send()
        if i < 7:
            dispatch(i).start()
        else:

            @pl.when(k == 1)
            def _():
                dispatch(7).start()

    @pl.when(k == 0)
    def _():
        x_buf[7] = out_buf[7]

    @pl.when(c == 1)
    def _():
        for dy in range(1, SIDE):
            for core in range(2):
                there = (ep, ((y + dy) % SIDE) * 2 + core)
                pl.semaphore_signal(plane_sem, inc=1, device_id=there, device_id_type=MESH)

    for copy in big:
        copy.wait()

    def hidden_of(rows_in, both):
        gate = jnp.dot(rows_in, both[0], preferred_element_type=jnp.float32)
        up = jnp.dot(rows_in, both[1], preferred_element_type=jnp.float32)
        return (gate / (1.0 + jnp.exp(-gate)) * up).astype(jnp.bfloat16)

    def give_back(i, dy, h):
        dz, dx = offset(k, i)
        own = i == 7 and dy == 0
        return pltpu.make_async_remote_copy(
            src_ref=y_buf.at[i, dy, h], dst_ref=r_buf.at[dy, (1 - k) * 8 + i],
            send_sem=r_send.at[h + 1 if own else 0 if i < 7 else 3],
            recv_sem=r_recv.at[4 * (1 - k) if own else dy],
            device_id=(chip(SIDE - dz, SIDE - dx), ((y + dy) % SIDE) * 2 + h), device_id_type=MESH,
        )

    for chunk, members in enumerate(CHUNKS):
        for i in members:
            if i < 7:
                dispatch(i).wait_recv()
            else:

                @pl.when(k == 1)
                def _():
                    dispatch(7).wait_recv()

        rows_in = jnp.concatenate([x_buf[i] for i in members], axis=0)
        hidden_own = hidden_of(rows_in, w_in)
        if chunk == 0:
            swaps[0].wait_recv()
            swaps[1].wait_recv()
        hidden_swap = hidden_of(rows_in, swap_in)
        if chunk == 0:
            swaps[2].wait_recv()
            pl.semaphore_wait(plane_sem, SIDE - 1)
        for group in GROUPS:
            for dy in group:
                for h in range(2):
                    cols = pl.ds(pl.multiple_of((((y + dy) % SIDE) * 2 + h) * BLK, BLK), BLK)
                    piece = jnp.dot(hidden_own, w_out[:, cols], preferred_element_type=jnp.float32)
                    piece += jnp.dot(hidden_swap, swap_out[:, cols], preferred_element_type=jnp.float32)
                    piece = piece.astype(jnp.bfloat16)
                    for n, i in enumerate(members):
                        y_buf[i, dy, h] = piece[n * CAP : (n + 1) * CAP]
            for dy, i, h in sending(group, members):
                if i < 7 or dy:
                    give_back(i, dy, h).start()
                else:
                    local = (k == 0) & (c == h)

                    @pl.when(local)
                    def _():
                        r_buf[0, 15] = y_buf[7, 0, h]

                    @pl.when(jnp.logical_not(local))
                    def _():
                        give_back(7, 0, h).start()

    scaled = jnp.where(here, weight, 0.0).T
    high = scaled.astype(jnp.bfloat16)
    low = (scaled - high.astype(jnp.float32)).astype(jnp.bfloat16)
    both = jnp.concatenate([high, low], axis=0)

    def arrived(blocks, sem):
        return pltpu.make_async_remote_copy(
            src_ref=blocks, dst_ref=blocks, send_sem=r_send.at[0], recv_sem=r_recv.at[sem],
            device_id=sibling, device_id_type=MESH,
        )

    arrived(r_buf.at[0, 0:15], 0).wait_recv()

    @pl.when(k == 1)
    def _():
        arrived(r_buf.at[0, 15], 4).wait_recv()

    for dy in (1, 3, 2):
        arrived(r_buf.at[dy], dy).wait_recv()
    twice = jnp.zeros((2 * rows, BLK), jnp.float32)
    for dy in range(SIDE):
        twice += jnp.dot(both, r_buf[dy].reshape(slots, BLK), preferred_element_type=jnp.float32)
    out_ref[...] = (twice[:rows] + twice[rows:]).astype(out_ref.dtype)

    for swap in swaps:
        swap.wait_send()
    for i in CHUNKS[1]:
        dispatch(i).wait_send()

    @pl.when(k == 1)
    def _():
        dispatch(7).wait_send()

    def sent(blocks, sem):
        return pltpu.make_async_remote_copy(
            src_ref=blocks, dst_ref=blocks, send_sem=r_send.at[sem], recv_sem=r_recv.at[0],
            device_id=sibling, device_id_type=MESH,
        )

    sent(y_buf.at[0:7], 0).wait_send()
    sent(y_buf.at[7, 1:4], 3).wait_send()
    for h in range(2):

        @pl.when(jnp.logical_not((k == 0) & (c == h)))
        def _():
            sent(y_buf.at[7, 0, h], h + 1).wait_send()


def body(tokens, norm_gain, norm_bias, routes, route_weights, gate_w, up_w, down_w):
    rows, width = tokens.shape
    half = gate_w.shape[2]
    hbm = pl.BlockSpec(memory_space=pltpu.HBM)
    bf16, f32 = jnp.bfloat16, jnp.float32
    dma = pltpu.SemaphoreType.DMA
    return pl.pallas_call(
        kernel,
        name="moe",
        out_shape=pltpu.VMEM((rows, BLK), bf16),
        in_specs=[hbm] * 8,
        out_specs=pl.BlockSpec(memory_space=pltpu.VMEM),
        scratch_shapes=[
            pltpu.VMEM((rows, width), bf16),
            pltpu.VMEM((1, width), f32),
            pltpu.VMEM((1, width), f32),
            pltpu.VMEM(routes.shape[::-1], jnp.int32),
            pltpu.VMEM(route_weights.shape[::-1], f32),
            pltpu.VMEM((2, width, half), bf16),
            pltpu.VMEM((half, width), bf16),
            pltpu.VMEM((2, width, half), bf16),
            pltpu.VMEM((half, width), bf16),
            pltpu.VMEM((8, CAP, width), bf16),
            pltpu.VMEM((8, CAP, width), bf16),
            pltpu.VMEM((8, SIDE, 2, CAP, BLK), bf16),
            pltpu.VMEM((SIDE, 16, CAP, BLK), bf16),
            dma((5,)), dma((3,)), dma((3,)), dma((3,)), dma((8,)), dma((8,)), dma((4,)), dma((5,)),
            pltpu.SemaphoreType.REGULAR,
            pltpu.SemaphoreType.REGULAR,
        ],
        compiler_params=pltpu.CompilerParams(collective_id=0, has_side_effects=True, vmem_limit_bytes=32 << 20),
    )(
        *(
            pltpu.with_memory_space_constraint(a, pltpu.HBM)
            for a in (
                tokens, norm_gain.reshape(1, width), norm_bias.reshape(1, width), routes.T, route_weights.T, gate_w, up_w, down_w
            )
        )
    )


def solution(mesh):
    placed = (
        P("ep", None),
        P(),
        P(),
        P("ep", None),
        P("ep", None),
        P("ep", None, "tp"),
        P("ep", None, "tp"),
        P("ep", "tp", None),
    )
    return jax.shard_map(body, mesh=mesh, in_specs=placed, out_specs=P("ep", "tp"), check_vma=False)
```

```python
import jax
import jax.numpy as jnp
from jax import lax
from jax.experimental import pallas as pl
from jax.experimental.pallas import tpu as pltpu
from jax.sharding import PartitionSpec as P

MESH = pl.DeviceIdType.MESH
SIDE = 4
CAP = 16
BLK = 256
CHUNKS = ((0, 1, 2, 7), (3, 4, 5, 6))
ORDER = (0, 1, 2, 7, 3, 4, 5, 6)
OFFSETS = (
    ((0, 3), (3, 0), (0, 2), (1, 3), (3, 1), (0, 1), (1, 0), (0, 0)),
    ((2, 2), (1, 2), (2, 1), (3, 2), (2, 3), (2, 0), (1, 1), (3, 3)),
)


RETURNS = (1, 3, 2, 0)


def offset(k, i):
    (z0, x0), (z1, x1) = OFFSETS[0][i], OFFSETS[1][i]
    return z0 + k * (z1 - z0), x0 + k * (x1 - x0)


def packed(which):
    word = 0
    for n, pair in enumerate(OFFSETS[1] + OFFSETS[0]):
        word |= pair[which] << (2 * n)
    return word - (1 << 32) if word >= 1 << 31 else word


def kernel(
    tok_hbm, gain_hbm, bias_hbm, routes_hbm, weights_hbm, gate_hbm, up_hbm, down_hbm,
    out_ref,
    tok, gain, bias, routes, weights, w_in, w_out, swap_in, swap_out,
    out_buf, x_buf, y_buf, r_buf,
    load_sem, wload_sem, swap_send, swap_recv, d_send, d_recv, r_send, r_recv, near_sem, plane_sem,
):
    ep, tp = lax.axis_index("ep"), lax.axis_index("tp")
    z, x = ep // SIDE, ep % SIDE
    y, c = tp // 2, tp % 2
    k = c

    def chip(dz, dx):
        return ((z + dz) % SIDE) * SIDE + (x + dx) % SIDE

    sibling = (ep, y * 2 + 1 - c)
    barrier = pltpu.get_barrier_semaphore()

    @pl.when(c == 1)
    def _():
        pl.semaphore_signal(barrier, inc=1, device_id=sibling, device_id_type=MESH)

    for dz, dx in sorted(OFFSETS[0][:7] + OFFSETS[1], key=lambda d: -min(d[0], 4 - d[0]) - min(d[1], 4 - d[1])):
        pl.semaphore_signal(barrier, inc=1, device_id=(chip(dz, dx), y * 2 + 1), device_id_type=MESH)
    for dy in range(1, SIDE):
        pl.semaphore_signal(barrier, inc=1, device_id=(ep, ((y + dy) % SIDE) * 2 + 1), device_id_type=MESH)

    small = [
        pltpu.make_async_copy(src, dst, load_sem.at[i])
        for i, (src, dst) in enumerate(
            ((tok_hbm, tok), (gain_hbm, gain), (bias_hbm, bias), (routes_hbm, routes), (weights_hbm, weights))
        )
    ]
    for copy in small:
        copy.start()
    big = [
        pltpu.make_async_copy(gate_hbm.at[0], w_in.at[0], wload_sem.at[0]),
        pltpu.make_async_copy(up_hbm.at[0], w_in.at[1], wload_sem.at[1]),
        pltpu.make_async_copy(down_hbm.at[0], w_out, wload_sem.at[2]),
    ]
    for copy in big:
        copy.start()

    @pl.when(c == 0)
    def _():
        pl.semaphore_wait(barrier, 1)
        pl.semaphore_signal(near_sem, inc=1, device_id=sibling, device_id_type=MESH)

    @pl.when(c == 1)
    def _():
        pl.semaphore_wait(near_sem, 1)

    def columns(dy, width):
        return pl.ds(pl.multiple_of(((y + dy) % SIDE) * width, width), width)

    swaps = [(gate_hbm.at[0], swap_in.at[0]), (up_hbm.at[0], swap_in.at[1])]
    for dy in RETURNS:
        swaps.append((down_hbm.at[0, :, columns(dy, 2 * BLK)], swap_out.at[:, columns(dy, 2 * BLK)]))
    swaps = [
        pltpu.make_async_remote_copy(
            src_ref=src, dst_ref=dst, send_sem=swap_send.at[i], recv_sem=swap_recv.at[i],
            device_id=sibling, device_id_type=MESH,
        )
        for i, (src, dst) in enumerate(swaps)
    ]
    for swap in swaps:
        swap.start()

    for copy in small:
        copy.wait()
    rows = tok.shape[0]
    values = tok[...].astype(jnp.float32)
    centred = values - jnp.mean(values, axis=-1, keepdims=True)
    variance = jnp.mean(centred * centred, axis=-1, keepdims=True)
    normed = (centred * lax.rsqrt(variance + 1e-05) * gain[...] + bias[...]).astype(jnp.bfloat16)

    slots = 16 * CAP
    slot = lax.broadcasted_iota(jnp.int32, (slots, rows), 0)
    shift = 2 * (slot // CAP)
    dz = lax.shift_right_logical(jnp.full_like(slot, packed(0)), shift) & 3
    dx = lax.shift_right_logical(jnp.full_like(slot, packed(1)), shift) & 3
    expert = ((z + dz) & 3) * SIDE + ((x + dx) & 3)
    named = jnp.zeros((slots, rows), jnp.float32)
    weight = jnp.zeros((slots, rows), jnp.float32)
    for i in range(routes.shape[0]):
        hit = routes[i : i + 1, :] == expert
        named = jnp.where(hit, 1.0, named)
        weight = jnp.where(hit, weights[i : i + 1, :], weight)
    earlier = (
        lax.broadcasted_iota(jnp.int32, (rows, rows), 0) < lax.broadcasted_iota(jnp.int32, (rows, rows), 1)
    ).astype(jnp.float32).astype(jnp.bfloat16)
    rank = jnp.dot(named.astype(jnp.bfloat16), earlier, preferred_element_type=jnp.float32)
    here = (named > 0.5) & (rank == (slot % CAP).astype(jnp.float32))
    picker = jnp.where(here, 1.0, 0.0)
    mine = jnp.where(k == 1, picker[: slots // 2], picker[slots // 2 :]).astype(jnp.bfloat16)
    outgoing = jnp.dot(mine, normed, preferred_element_type=jnp.float32)
    out_buf[...] = outgoing.astype(jnp.bfloat16).reshape(out_buf.shape)

    @pl.when(c == 1)
    def _():
        pl.semaphore_wait(barrier, 2 * (SIDE * SIDE - 1 + SIDE - 1))
        pl.semaphore_signal(near_sem, inc=1, device_id=sibling, device_id_type=MESH)

    @pl.when(c == 0)
    def _():
        pl.semaphore_wait(near_sem, 1)

    def dispatch(i):
        dz, dx = offset(k, i)
        return pltpu.make_async_remote_copy(
            src_ref=out_buf.at[i], dst_ref=x_buf.at[i], send_sem=d_send.at[i], recv_sem=d_recv.at[i],
            device_id=(chip(dz, dx), y * 2 + c), device_id_type=MESH,
        )

    for i in ORDER:
        if i == CHUNKS[1][0]:
            for n in CHUNKS[0]:
                if n < 7:
                    dispatch(n).wait_send()
        if i < 7:
            dispatch(i).start()
        else:

            @pl.when(k == 1)
            def _():
                dispatch(7).start()

    @pl.when(k == 0)
    def _():
        x_buf[7] = out_buf[7]

    @pl.when(c == 1)
    def _():
        for dy in range(1, SIDE):
            for core in range(2):
                there = (ep, ((y + dy) % SIDE) * 2 + core)
                pl.semaphore_signal(plane_sem, inc=1, device_id=there, device_id_type=MESH)

    for copy in big:
        copy.wait()

    def hidden_of(rows_in, both):
        gate = jnp.dot(rows_in, both[0], preferred_element_type=jnp.float32)
        up = jnp.dot(rows_in, both[1], preferred_element_type=jnp.float32)
        return (gate / (1.0 + jnp.exp(-gate)) * up).astype(jnp.bfloat16)

    def give_back(i, dy, h):
        dz, dx = offset(k, i)
        own = i == 7 and dy == 0
        return pltpu.make_async_remote_copy(
            src_ref=y_buf.at[i, dy, h], dst_ref=r_buf.at[dy, (1 - k) * 8 + i],
            send_sem=r_send.at[h + 1 if own else 0 if i < 7 else 3],
            recv_sem=r_recv.at[4 * (1 - k) if own else dy],
            device_id=(chip(SIDE - dz, SIDE - dx), ((y + dy) % SIDE) * 2 + h), device_id_type=MESH,
        )

    for chunk, members in enumerate(CHUNKS):
        for i in members:
            if i < 7:
                dispatch(i).wait_recv()
            else:

                @pl.when(k == 1)
                def _():
                    dispatch(7).wait_recv()

        rows_in = jnp.concatenate([x_buf[i] for i in members], axis=0)
        hidden_own = hidden_of(rows_in, w_in)
        if chunk == 0:
            swaps[0].wait_recv()
            swaps[1].wait_recv()
        hidden_swap = hidden_of(rows_in, swap_in)
        if chunk == 0:
            pl.semaphore_wait(plane_sem, SIDE - 1)
        for step, dy in enumerate(RETURNS):
            if chunk == 0:
                swaps[2 + step].wait_recv()
            for h in range(2):
                cols = pl.ds(pl.multiple_of((((y + dy) % SIDE) * 2 + h) * BLK, BLK), BLK)
                piece = jnp.dot(hidden_own, w_out[:, cols], preferred_element_type=jnp.float32)
                piece += jnp.dot(hidden_swap, swap_out[:, cols], preferred_element_type=jnp.float32)
                piece = piece.astype(jnp.bfloat16)
                for n, i in enumerate(members):
                    y_buf[i, dy, h] = piece[n * CAP : (n + 1) * CAP]
            for i in members:
                for h in range(2):
                    if i < 7 or dy:
                        give_back(i, dy, h).start()
                    else:
                        local = (k == 0) & (c == h)

                        @pl.when(local)
                        def _():
                            r_buf[0, 15] = y_buf[7, 0, h]

                        @pl.when(jnp.logical_not(local))
                        def _():
                            give_back(7, 0, h).start()

    scaled = jnp.where(here, weight, 0.0).T
    high = scaled.astype(jnp.bfloat16)
    low = (scaled - high.astype(jnp.float32)).astype(jnp.bfloat16)
    both = jnp.concatenate([high, low], axis=0)

    def arrived(blocks, sem):
        return pltpu.make_async_remote_copy(
            src_ref=blocks, dst_ref=blocks, send_sem=r_send.at[0], recv_sem=r_recv.at[sem],
            device_id=sibling, device_id_type=MESH,
        )

    twice = jnp.zeros((2 * rows, BLK), jnp.float32)
    for dy in (1, 3, 2, 0):
        if dy:
            arrived(r_buf.at[dy], dy).wait_recv()
        else:
            arrived(r_buf.at[0, 0:15], 0).wait_recv()

            @pl.when(k == 1)
            def _():
                arrived(r_buf.at[0, 15], 4).wait_recv()

        twice += jnp.dot(both, r_buf[dy].reshape(slots, BLK), preferred_element_type=jnp.float32)
    out_ref[...] = (twice[:rows] + twice[rows:]).astype(out_ref.dtype)

    for swap in swaps:
        swap.wait_send()
    for i in CHUNKS[1]:
        dispatch(i).wait_send()

    @pl.when(k == 1)
    def _():
        dispatch(7).wait_send()

    def sent(blocks, sem):
        return pltpu.make_async_remote_copy(
            src_ref=blocks, dst_ref=blocks, send_sem=r_send.at[sem], recv_sem=r_recv.at[0],
            device_id=sibling, device_id_type=MESH,
        )

    sent(y_buf.at[0:7], 0).wait_send()
    sent(y_buf.at[7, 1:4], 3).wait_send()
    for h in range(2):

        @pl.when(jnp.logical_not((k == 0) & (c == h)))
        def _():
            sent(y_buf.at[7, 0, h], h + 1).wait_send()


def body(tokens, norm_gain, norm_bias, routes, route_weights, gate_w, up_w, down_w):
    rows, width = tokens.shape
    half = gate_w.shape[2]
    hbm = pl.BlockSpec(memory_space=pltpu.HBM)
    bf16, f32 = jnp.bfloat16, jnp.float32
    dma = pltpu.SemaphoreType.DMA
    return pl.pallas_call(
        kernel,
        name="moe",
        out_shape=pltpu.VMEM((rows, BLK), bf16),
        in_specs=[hbm] * 8,
        out_specs=pl.BlockSpec(memory_space=pltpu.VMEM),
        scratch_shapes=[
            pltpu.VMEM((rows, width), bf16),
            pltpu.VMEM((1, width), f32),
            pltpu.VMEM((1, width), f32),
            pltpu.VMEM(routes.shape[::-1], jnp.int32),
            pltpu.VMEM(route_weights.shape[::-1], f32),
            pltpu.VMEM((2, width, half), bf16),
            pltpu.VMEM((half, width), bf16),
            pltpu.VMEM((2, width, half), bf16),
            pltpu.VMEM((half, width), bf16),
            pltpu.VMEM((8, CAP, width), bf16),
            pltpu.VMEM((8, CAP, width), bf16),
            pltpu.VMEM((8, SIDE, 2, CAP, BLK), bf16),
            pltpu.VMEM((SIDE, 16, CAP, BLK), bf16),
            dma((5,)), dma((3,)), dma((6,)), dma((6,)), dma((8,)), dma((8,)), dma((4,)), dma((5,)),
            pltpu.SemaphoreType.REGULAR,
            pltpu.SemaphoreType.REGULAR,
        ],
        compiler_params=pltpu.CompilerParams(collective_id=0, has_side_effects=True, vmem_limit_bytes=32 << 20),
    )(
        *(
            pltpu.with_memory_space_constraint(a, pltpu.HBM)
            for a in (
                tokens, norm_gain.reshape(1, width), norm_bias.reshape(1, width), routes.T, route_weights.T, gate_w, up_w, down_w
            )
        )
    )


def solution(mesh):
    placed = (
        P("ep", None),
        P(),
        P(),
        P("ep", None),
        P("ep", None),
        P("ep", None, "tp"),
        P("ep", None, "tp"),
        P("ep", "tp", None),
    )
    return jax.shard_map(body, mesh=mesh, in_specs=placed, out_specs=P("ep", "tp"), check_vma=False)
```

```python
import jax
import jax.numpy as jnp
from jax import lax
from jax.experimental import pallas as pl
from jax.experimental.pallas import tpu as pltpu
from jax.sharding import PartitionSpec as P

MESH = pl.DeviceIdType.MESH
SIDE = 4
CAP = 16
BLK = 256
CHUNKS = ((0, 1, 2, 7), (3, 4, 5, 6))
ORDER = (0, 1, 2, 7, 3, 4, 5, 6)
OFFSETS = (
    ((0, 3), (3, 0), (0, 2), (1, 3), (3, 1), (0, 1), (1, 0), (0, 0)),
    ((2, 2), (1, 2), (2, 1), (3, 2), (2, 3), (2, 0), (1, 1), (3, 3)),
)


RETURNS = (1, 3, 2, 0)


def offset(k, i):
    (z0, x0), (z1, x1) = OFFSETS[0][i], OFFSETS[1][i]
    return z0 + k * (z1 - z0), x0 + k * (x1 - x0)


def packed(which):
    word = 0
    for n, pair in enumerate(OFFSETS[1] + OFFSETS[0]):
        word |= pair[which] << (2 * n)
    return word - (1 << 32) if word >= 1 << 31 else word


def kernel(
    tok_hbm, gain_hbm, bias_hbm, routes_hbm, weights_hbm, gate_hbm, up_hbm, down_hbm,
    out_ref,
    tok, gain, bias, routes, weights, w_in, w_out, swap_in, swap_out,
    out_buf, x_buf, y_buf, r_buf,
    load_sem, wload_sem, swap_send, swap_recv, d_send, d_recv, r_send, r_recv, near_sem, plane_sem,
):
    ep, tp = lax.axis_index("ep"), lax.axis_index("tp")
    z, x = ep // SIDE, ep % SIDE
    y, c = tp // 2, tp % 2
    k = c

    def chip(dz, dx):
        return ((z + dz) % SIDE) * SIDE + (x + dx) % SIDE

    sibling = (ep, y * 2 + 1 - c)
    small = [
        pltpu.make_async_copy(src, dst, load_sem.at[i])
        for i, (src, dst) in enumerate(
            ((tok_hbm, tok), (gain_hbm, gain), (bias_hbm, bias), (routes_hbm, routes), (weights_hbm, weights))
        )
    ]
    for copy in small:
        copy.start()

    barrier = pltpu.get_barrier_semaphore()

    @pl.when(c == 1)
    def _():
        pl.semaphore_signal(barrier, inc=1, device_id=sibling, device_id_type=MESH)

    for dz, dx in sorted(OFFSETS[0][:7] + OFFSETS[1], key=lambda d: -min(d[0], 4 - d[0]) - min(d[1], 4 - d[1])):
        pl.semaphore_signal(barrier, inc=1, device_id=(chip(dz, dx), y * 2 + 1), device_id_type=MESH)
    for dy in range(1, SIDE):
        pl.semaphore_signal(barrier, inc=1, device_id=(ep, ((y + dy) % SIDE) * 2 + 1), device_id_type=MESH)

    big = [
        pltpu.make_async_copy(gate_hbm.at[0], w_in.at[0], wload_sem.at[0]),
        pltpu.make_async_copy(up_hbm.at[0], w_in.at[1], wload_sem.at[1]),
        pltpu.make_async_copy(down_hbm.at[0], w_out, wload_sem.at[2]),
    ]
    for copy in big:
        copy.start()

    @pl.when(c == 0)
    def _():
        pl.semaphore_wait(barrier, 1)
        pl.semaphore_signal(near_sem, inc=1, device_id=sibling, device_id_type=MESH)

    @pl.when(c == 1)
    def _():
        pl.semaphore_wait(near_sem, 1)

    def columns(dy, width):
        return pl.ds(pl.multiple_of(((y + dy) % SIDE) * width, width), width)

    swaps = [(gate_hbm.at[0], swap_in.at[0]), (up_hbm.at[0], swap_in.at[1])]
    for dy in RETURNS:
        swaps.append((down_hbm.at[0, :, columns(dy, 2 * BLK)], swap_out.at[:, columns(dy, 2 * BLK)]))
    swaps = [
        pltpu.make_async_remote_copy(
            src_ref=src, dst_ref=dst, send_sem=swap_send.at[i], recv_sem=swap_recv.at[i],
            device_id=sibling, device_id_type=MESH,
        )
        for i, (src, dst) in enumerate(swaps)
    ]
    for swap in swaps:
        swap.start()

    for copy in small:
        copy.wait()
    rows = tok.shape[0]
    values = tok[...].astype(jnp.float32)
    centred = values - jnp.mean(values, axis=-1, keepdims=True)
    variance = jnp.mean(centred * centred, axis=-1, keepdims=True)
    normed = (centred * lax.rsqrt(variance + 1e-05) * gain[...] + bias[...]).astype(jnp.bfloat16)

    slots = 16 * CAP
    slot = lax.broadcasted_iota(jnp.int32, (slots, rows), 0)
    shift = 2 * (slot // CAP)
    dz = lax.shift_right_logical(jnp.full_like(slot, packed(0)), shift) & 3
    dx = lax.shift_right_logical(jnp.full_like(slot, packed(1)), shift) & 3
    expert = ((z + dz) & 3) * SIDE + ((x + dx) & 3)
    named = jnp.zeros((slots, rows), jnp.float32)
    weight = jnp.zeros((slots, rows), jnp.float32)
    for i in range(routes.shape[0]):
        hit = routes[i : i + 1, :] == expert
        named = jnp.where(hit, 1.0, named)
        weight = jnp.where(hit, weights[i : i + 1, :], weight)
    earlier = (
        lax.broadcasted_iota(jnp.int32, (rows, rows), 0) < lax.broadcasted_iota(jnp.int32, (rows, rows), 1)
    ).astype(jnp.float32).astype(jnp.bfloat16)
    rank = jnp.dot(named.astype(jnp.bfloat16), earlier, preferred_element_type=jnp.float32)
    here = (named > 0.5) & (rank == (slot % CAP).astype(jnp.float32))
    picker = jnp.where(here, 1.0, 0.0)
    mine = jnp.where(k == 1, picker[: slots // 2], picker[slots // 2 :]).astype(jnp.bfloat16)
    outgoing = jnp.dot(mine, normed, preferred_element_type=jnp.float32)
    out_buf[...] = outgoing.astype(jnp.bfloat16).reshape(out_buf.shape)

    @pl.when(c == 1)
    def _():
        pl.semaphore_wait(barrier, 2 * (SIDE * SIDE - 1 + SIDE - 1))
        pl.semaphore_signal(near_sem, inc=1, device_id=sibling, device_id_type=MESH)

    @pl.when(c == 0)
    def _():
        pl.semaphore_wait(near_sem, 1)

    def dispatch(i):
        dz, dx = offset(k, i)
        return pltpu.make_async_remote_copy(
            src_ref=out_buf.at[i], dst_ref=x_buf.at[i], send_sem=d_send.at[i], recv_sem=d_recv.at[i],
            device_id=(chip(dz, dx), y * 2 + c), device_id_type=MESH,
        )

    for i in ORDER:
        if i == CHUNKS[1][0]:
            for n in CHUNKS[0]:
                if n < 7:
                    dispatch(n).wait_send()
        if i < 7:
            dispatch(i).start()
        else:

            @pl.when(k == 1)
            def _():
                dispatch(7).start()

    @pl.when(k == 0)
    def _():
        x_buf[7] = out_buf[7]

    @pl.when(c == 1)
    def _():
        for dy in range(1, SIDE):
            for core in range(2):
                there = (ep, ((y + dy) % SIDE) * 2 + core)
                pl.semaphore_signal(plane_sem, inc=1, device_id=there, device_id_type=MESH)

    for copy in big:
        copy.wait()

    def hidden_of(rows_in, both):
        gate = jnp.dot(rows_in, both[0], preferred_element_type=jnp.float32)
        up = jnp.dot(rows_in, both[1], preferred_element_type=jnp.float32)
        return (gate / (1.0 + jnp.exp(-gate)) * up).astype(jnp.bfloat16)

    def give_back(i, dy, h):
        dz, dx = offset(k, i)
        own = i == 7 and dy == 0
        return pltpu.make_async_remote_copy(
            src_ref=y_buf.at[i, dy, h], dst_ref=r_buf.at[dy, (1 - k) * 8 + i],
            send_sem=r_send.at[h + 1 if own else 0 if i < 7 else 3],
            recv_sem=r_recv.at[4 * (1 - k) if own else dy],
            device_id=(chip(SIDE - dz, SIDE - dx), ((y + dy) % SIDE) * 2 + h), device_id_type=MESH,
        )

    for chunk, members in enumerate(CHUNKS):
        for i in members:
            if i < 7:
                dispatch(i).wait_recv()
            else:

                @pl.when(k == 1)
                def _():
                    dispatch(7).wait_recv()

        rows_in = jnp.concatenate([x_buf[i] for i in members], axis=0)
        hidden_own = hidden_of(rows_in, w_in)
        if chunk == 0:
            swaps[0].wait_recv()
            swaps[1].wait_recv()
        hidden_swap = hidden_of(rows_in, swap_in)
        if chunk == 0:
            pl.semaphore_wait(plane_sem, SIDE - 1)
        for step, dy in enumerate(RETURNS):
            if chunk == 0:
                swaps[2 + step].wait_recv()
            for h in range(2):
                cols = pl.ds(pl.multiple_of((((y + dy) % SIDE) * 2 + h) * BLK, BLK), BLK)
                piece = jnp.dot(hidden_own, w_out[:, cols], preferred_element_type=jnp.float32)
                piece += jnp.dot(hidden_swap, swap_out[:, cols], preferred_element_type=jnp.float32)
                piece = piece.astype(jnp.bfloat16)
                for n, i in enumerate(members):
                    y_buf[i, dy, h] = piece[n * CAP : (n + 1) * CAP]
            for i in members:
                for h in range(2):
                    if i < 7 or dy:
                        give_back(i, dy, h).start()
                    else:
                        local = (k == 0) & (c == h)

                        @pl.when(local)
                        def _():
                            r_buf[0, 15] = y_buf[7, 0, h]

                        @pl.when(jnp.logical_not(local))
                        def _():
                            give_back(7, 0, h).start()

    scaled = jnp.where(here, weight, 0.0).T
    high = scaled.astype(jnp.bfloat16)
    low = (scaled - high.astype(jnp.float32)).astype(jnp.bfloat16)
    both = jnp.concatenate([high, low], axis=0)

    def arrived(blocks, sem):
        return pltpu.make_async_remote_copy(
            src_ref=blocks, dst_ref=blocks, send_sem=r_send.at[0], recv_sem=r_recv.at[sem],
            device_id=sibling, device_id_type=MESH,
        )

    twice = jnp.zeros((2 * rows, BLK), jnp.float32)
    for dy in (1, 3, 2, 0):
        if dy:
            arrived(r_buf.at[dy], dy).wait_recv()
        else:
            arrived(r_buf.at[0, 0:15], 0).wait_recv()

            @pl.when(k == 1)
            def _():
                arrived(r_buf.at[0, 15], 4).wait_recv()

        twice += jnp.dot(both, r_buf[dy].reshape(slots, BLK), preferred_element_type=jnp.float32)
    out_ref[...] = (twice[:rows] + twice[rows:]).astype(out_ref.dtype)

    for swap in swaps:
        swap.wait_send()
    for i in CHUNKS[1]:
        dispatch(i).wait_send()

    @pl.when(k == 1)
    def _():
        dispatch(7).wait_send()

    def sent(blocks, sem):
        return pltpu.make_async_remote_copy(
            src_ref=blocks, dst_ref=blocks, send_sem=r_send.at[sem], recv_sem=r_recv.at[0],
            device_id=sibling, device_id_type=MESH,
        )

    sent(y_buf.at[0:7], 0).wait_send()
    sent(y_buf.at[7, 1:4], 3).wait_send()
    for h in range(2):

        @pl.when(jnp.logical_not((k == 0) & (c == h)))
        def _():
            sent(y_buf.at[7, 0, h], h + 1).wait_send()


def body(tokens, norm_gain, norm_bias, routes, route_weights, gate_w, up_w, down_w):
    rows, width = tokens.shape
    half = gate_w.shape[2]
    hbm = pl.BlockSpec(memory_space=pltpu.HBM)
    bf16, f32 = jnp.bfloat16, jnp.float32
    dma = pltpu.SemaphoreType.DMA
    return pl.pallas_call(
        kernel,
        name="moe",
        out_shape=pltpu.VMEM((rows, BLK), bf16),
        in_specs=[hbm] * 8,
        out_specs=pl.BlockSpec(memory_space=pltpu.VMEM),
        scratch_shapes=[
            pltpu.VMEM((rows, width), bf16),
            pltpu.VMEM((1, width), f32),
            pltpu.VMEM((1, width), f32),
            pltpu.VMEM(routes.shape[::-1], jnp.int32),
            pltpu.VMEM(route_weights.shape[::-1], f32),
            pltpu.VMEM((2, width, half), bf16),
            pltpu.VMEM((half, width), bf16),
            pltpu.VMEM((2, width, half), bf16),
            pltpu.VMEM((half, width), bf16),
            pltpu.VMEM((8, CAP, width), bf16),
            pltpu.VMEM((8, CAP, width), bf16),
            pltpu.VMEM((8, SIDE, 2, CAP, BLK), bf16),
            pltpu.VMEM((SIDE, 16, CAP, BLK), bf16),
            dma((5,)), dma((3,)), dma((6,)), dma((6,)), dma((8,)), dma((8,)), dma((4,)), dma((5,)),
            pltpu.SemaphoreType.REGULAR,
            pltpu.SemaphoreType.REGULAR,
        ],
        compiler_params=pltpu.CompilerParams(collective_id=0, has_side_effects=True, vmem_limit_bytes=32 << 20),
    )(
        *(
            pltpu.with_memory_space_constraint(a, pltpu.HBM)
            for a in (
                tokens, norm_gain.reshape(1, width), norm_bias.reshape(1, width), routes.T, route_weights.T, gate_w, up_w, down_w
            )
        )
    )


def solution(mesh):
    placed = (
        P("ep", None),
        P(),
        P(),
        P("ep", None),
        P("ep", None),
        P("ep", None, "tp"),
        P("ep", None, "tp"),
        P("ep", "tp", None),
    )
    return jax.shard_map(body, mesh=mesh, in_specs=placed, out_specs=P("ep", "tp"), check_vma=False)
```
